32 devices in a mesh: grp: 2 (over y), sp: 4 (over z), tp: 4 (over x, core).
Axes of the slice: x: 2, y: 2, z: 4, core: 2. Of those that a mesh axis runs over, the one named last changes fastest.
Arguments:
- source: bfloat16 [4096, 2048], P(('grp', 'sp', 'tp')), parts along dimension 0, may hold values from -8 to 8
- target: bfloat16 [1024, 2048], P(('grp', 'sp', 'tp')), parts along dimension 0, may hold values from -8 to 8
- source_gain: float32 [2048], replicated, may hold values from 0.1 to 1.9
- attend_gain: float32 [2, 2048], replicated, may hold values from 0.1 to 1.9
- query_weight: bfloat16 [2, 2048, 2048], P(None, None, 'tp'), may hold values from -4 to 4
- key_weight: bfloat16 [2, 2048, 2048], P(None, None, 'tp'), may hold values from -4 to 4
- value_weight: bfloat16 [2, 2048, 2048], P(None, None, 'tp'), may hold values from -0.125 to 0.125
- out_weight: bfloat16 [2, 2048, 2048], P(None, 'tp'), may hold values from -3 to 3
- mixer_gain: float32 [2048], replicated, may hold values from 0.1 to 1.9
- gate_weight: bfloat16 [2048, 2816], P(None, 'tp'), may hold values from -0.125 to 0.125
- up_weight: bfloat16 [2048, 2816], P(None, 'tp'), may hold values from -0.125 to 0.125
- gate_taps: float32 [3, 2816], P(None, 'tp'), may hold values from -3 to 3
- up_taps: float32 [3, 2816], P(None, 'tp'), may hold values from -3 to 3
- down_weight: bfloat16 [2816, 2048], P('tp'), may hold values from -0.109375 to 0.109375
- final_gain: float32 [2048], replicated, may hold values from 0.1 to 1.9
Outputs:
- result: bfloat16 [1024, 2048], P(('grp', 'sp', 'tp')), parts along dimension 0
The draws below stay inside these ranges and needn't reach their ends.
There are 2 independent parts, one for each index of `grp`. The reference program is written for one: setup_inputs(seed, part) draws one part's arguments, and reference() takes and returns one part's arrays. A program takes and returns all parts, laid end to end along the dimension named above; an argument that names none is the same for every part. Nothing has to cross between parts.
All inputs are finite; a program needn't handle non-finite values.
Results may differ from the reference program's by a relative error of at most 0.04.
Values may be sent and summed in bfloat16 or wider, within the bound.
A program may use at most 128 MiB of HBM per device.

```python
import jax
import jax.numpy as jnp
from jax import lax

D = 2048
HEADS = 8
FF = 2816
HD = 256
SRC = 2048
TGT = 512


def projection_draw(key, salt_value):
    stacked = []
    for layer_number in range(2):
        base_draw = jax.random.normal(jax.random.fold_in(key, salt_value * 10 + layer_number), (D, D), jnp.float32)
        layer_matrix = jnp.clip(base_draw, -6.0, 6.0) * D ** (-0.5)
        stacked.append(jnp.clip(layer_matrix, -4.0, 4.0))
    return jnp.stack(stacked).astype(jnp.bfloat16)


def row_draw(key, row_count):
    base_rows = jnp.clip(jax.random.normal(jax.random.fold_in(key, 1), (row_count, D), jnp.float32), -6.0, 6.0)
    return base_rows.astype(jnp.bfloat16)


def draw_source(key, part):
    return row_draw(key, SRC)


def draw_target(key, part):
    return row_draw(key, TGT)


def draw_query_weight(key, part):
    return projection_draw(key, 1)


def draw_key_weight(key, part):
    return projection_draw(key, 2)


def steps_of(own_key, shape, pieces, low, largest):
    level = 1.0
    for position, shards_of in pieces:
        draws = jax.random.uniform(jax.random.fold_in(jax.random.fold_in(own_key, 6), position), (shards_of,), jnp.float32, low / len(pieces), largest / len(pieces))
        level = level * jnp.repeat(jnp.exp(draws), shape[position] // shards_of).reshape((-1,) + (1,) * (len(shape) - 1 - position))
    return level


def centred(rng, extent, width, limit, split=(), kind=jnp.bfloat16):
    level = steps_of(rng, extent, split, -0.22, 0.18) if split else 1.0
    entries = jax.random.normal(rng, extent, jnp.float32) * width * level
    return jnp.minimum(jnp.maximum(entries, -limit), limit).astype(kind)


def setup_inputs(seed: int = 0, part: int = 0) -> dict:
    keys = jax.random.split(jax.random.key(seed), 16)
    own_keys = jax.random.split(jax.random.fold_in(keys[15], part), 16)
    return {
        "source": draw_source(jax.random.fold_in(jax.random.fold_in(keys[15], part), 71), part),
        "target": draw_target(jax.random.fold_in(jax.random.fold_in(keys[15], part), 71), part),
        "source_gain": jnp.clip(1.0 + 0.18 * jax.random.normal(keys[2], (D,), jnp.float32), 0.1, 1.9),
        "attend_gain": jnp.clip(1.0 + 0.18 * jax.random.normal(keys[3], (2, D), jnp.float32), 0.1, 1.9),
        "query_weight": draw_query_weight(jax.random.fold_in(keys[15], 71), part),
        "key_weight": draw_key_weight(jax.random.fold_in(keys[15], 71), part),
        "value_weight": centred(keys[6], (2, D, D), D ** -0.5, 0.125, ((2, 4),)),
        "out_weight": centred(keys[7], (2, D, D), 4 ** -0.5, 3.0, ((1, 4),)),
        "mixer_gain": jnp.clip(1.0 + 0.18 * jax.random.normal(keys[8], (D,), jnp.float32), 0.1, 1.9),
        "gate_weight": centred(keys[9], (D, FF), D ** -0.5, 0.125, ((1, 4),)),
        "up_weight": centred(keys[10], (D, FF), D ** -0.5, 0.125, ((1, 4),)),
        "gate_taps": centred(keys[11], (3, FF), 0.6, 3.0, ((1, 4),), jnp.float32),
        "up_taps": centred(keys[12], (3, FF), 0.6, 3.0, ((1, 4),), jnp.float32),
        "down_weight": centred(keys[13], (FF, D), FF ** -0.5, 0.109375, ((0, 4),)),
        "final_gain": jnp.clip(1.0 + 0.18 * jax.random.normal(keys[14], (D,), jnp.float32), 0.1, 1.9),
    }


EPS = 1e-06

def normed_rows(rows, gain):
    wide = rows.astype(jnp.float32)
    return wide * lax.rsqrt(lax.optimization_barrier(jnp.mean(wide * wide, axis=-1, keepdims=True)) + EPS) * gain

def one_head(triple):
    query_head, key_head, value_head = triple
    scores = jnp.dot(query_head, key_head.T, preferred_element_type=jnp.float32) * HD ** (-0.5)
    highest = lax.optimization_barrier(jnp.max(scores, axis=-1, keepdims=True))
    raised = jnp.exp(scores - highest)
    totals = lax.optimization_barrier(jnp.sum(raised, axis=-1, keepdims=True))
    weights = raised.astype(jnp.bfloat16)
    summed = jnp.dot(weights, value_head, preferred_element_type=jnp.float32)
    return (summed / totals).astype(jnp.bfloat16)

def split_heads(block):
    return block.reshape(block.shape[0], HEADS, HD).transpose(1, 0, 2)

def reference(source, target, source_gain, attend_gain, query_weight, key_weight, value_weight, out_weight, mixer_gain, gate_weight, up_weight, gate_taps, up_taps, down_weight, final_gain):
    source_normed = normed_rows(source, source_gain).astype(jnp.bfloat16)
    residual = target.astype(jnp.float32)
    for layer_number in range(2):
        normed = normed_rows(residual, attend_gain[layer_number]).astype(jnp.bfloat16)
        query_block = jnp.dot(normed, query_weight[layer_number], preferred_element_type=jnp.float32).astype(jnp.bfloat16)
        key_rows = jnp.dot(source_normed, key_weight[layer_number], preferred_element_type=jnp.float32).astype(jnp.bfloat16)
        value_rows = jnp.dot(source_normed, value_weight[layer_number], preferred_element_type=jnp.float32).astype(jnp.bfloat16)
        attended = lax.map(one_head, (split_heads(query_block), split_heads(key_rows), split_heads(value_rows)))
        attended = attended.transpose(1, 0, 2).reshape(query_block.shape[0], D)
        residual = residual + jnp.dot(attended, out_weight[layer_number], preferred_element_type=jnp.float32)
    mixed = normed_rows(residual, mixer_gain).astype(jnp.bfloat16)
    gated = jnp.dot(mixed, gate_weight, preferred_element_type=jnp.float32).astype(jnp.bfloat16)
    upped = jnp.dot(mixed, up_weight, preferred_element_type=jnp.float32).astype(jnp.bfloat16)
    zero_rows = jnp.zeros((2, FF), jnp.float32)
    gate_pad = jnp.concatenate([zero_rows, gated.astype(jnp.float32)], axis=0)
    up_pad = jnp.concatenate([zero_rows, upped.astype(jnp.float32)], axis=0)
    gate_conv = gate_taps[0] * gate_pad[:-2] + gate_taps[1] * gate_pad[1:-1] + gate_taps[2] * gate_pad[2:]
    up_conv = up_taps[0] * up_pad[:-2] + up_taps[1] * up_pad[1:-1] + up_taps[2] * up_pad[2:]
    hidden = (jax.nn.silu(gate_conv) * up_conv).astype(jnp.bfloat16)
    residual = residual + jnp.dot(hidden, down_weight, preferred_element_type=jnp.float32)
    return normed_rows(residual, final_gain).astype(jnp.bfloat16)
```

```python
import functools

import jax
import jax.numpy as jnp
from jax import lax
from jax.experimental import pallas as pl
from jax.experimental.pallas import tpu as pltpu
from jax.sharding import PartitionSpec as P

HD = 256
EPS = 1e-06
TILE = 256
STAT_ROWS = 8
LANES = 128
MESH = pl.DeviceIdType.MESH
BF = jnp.bfloat16
F32 = jnp.float32


def normed_rows(wide, gain):
    return wide * lax.rsqrt(jnp.mean(wide * wide, axis=-1, keepdims=True) + EPS) * gain


def mm(a, b):
    return jnp.dot(a, b, preferred_element_type=F32)


def kernel(
    n,
    S,
    source,
    target,
    source_gain,
    attend_gain,
    query_weight,
    key_weight,
    value_weight,
    out_weight,
    mixer_gain,
    gate_weight,
    up_weight,
    gate_taps,
    up_taps,
    down_weight,
    final_gain,
    result,
    sv,
    tv,
    wq,
    wkv,
    wo,
    wg,
    wu,
    wd,
    xs,
    xt,
    kv,
    qall,
    osend,
    orecv,
    ssend,
    srecv,
    pf,
    att,
    p1s,
    p1r,
    p2s,
    p2r,
    hs,
    hr,
    gpad,
    upad,
    hid,
    residual,
    load_sem,
    w_sem,
    ag_send,
    ag_recv,
    q_send,
    q_recv,
    r_send,
    r_recv,
    s_send,
    s_recv,
    p1_send,
    p1_recv,
    p2_send,
    p2_recv,
    h_send,
    h_recv,
):
    X = n // 2
    Rs, D = source.shape
    Rt = target.shape[0]
    W = wq.shape[2]
    T = n * Rt
    heads = W // HD
    F = wg.shape[1]
    scale = HD ** (-0.5)
    t = lax.axis_index("tp")
    s = lax.axis_index("sp")
    x = lax.div(t, 2)
    c = lax.rem(t, 2)
    other = 1 - c
    peer = x * 2 + other
    pending = []

    def tp_at(k):
        return lax.rem(x + k, X)

    def tp_from(k):
        return lax.rem(x + X - k, X)

    def sp_at(i):
        return lax.rem(s + i, S)

    def remote(src, dst, ss, rs, axis, where):
        return pltpu.make_async_remote_copy(
            src_ref=src,
            dst_ref=dst,
            send_sem=ss,
            recv_sem=rs,
            device_id={axis: where},
            device_id_type=MESH,
        )

    def launch(copy):
        copy.start()
        pending.append(copy)

    barrier = pltpu.get_barrier_semaphore()
    pl.semaphore_signal(barrier, inc=1, device_id={"tp": peer}, device_id_type=MESH)
    for k in range(1, X):
        pl.semaphore_signal(
            barrier, inc=1, device_id={"tp": tp_at(k) * 2 + c}, device_id_type=MESH
        )
    for i in range(1, S):
        pl.semaphore_signal(barrier, inc=1, device_id={"sp": sp_at(i)}, device_id_type=MESH)

    load_t = pltpu.make_async_copy(target, tv, load_sem.at[0])
    load_s = pltpu.make_async_copy(source, sv, load_sem.at[1])
    load_t.start()
    load_s.start()
    load_q = [pltpu.make_async_copy(query_weight.at[l], wq.at[l], w_sem.at[l]) for l in range(2)]
    load_kv = []
    for l in range(2):
        load_kv.append(
            [
                pltpu.make_async_copy(key_weight.at[l], wkv.at[2 * l], w_sem.at[2 + 2 * l]),
                pltpu.make_async_copy(value_weight.at[l], wkv.at[2 * l + 1], w_sem.at[3 + 2 * l]),
            ]
        )
    load_o = [pltpu.make_async_copy(out_weight.at[l], wo.at[l], w_sem.at[6 + l]) for l in range(2)]
    load_m = [
        pltpu.make_async_copy(gate_weight, wg, w_sem.at[8]),
        pltpu.make_async_copy(up_weight, wu, w_sem.at[9]),
        pltpu.make_async_copy(down_weight, wd, w_sem.at[10]),
    ]
    for copy in [load_q[0], *load_kv[0], *load_kv[1], load_o[0], load_q[1], load_o[1], *load_m]:
        copy.start()

    def gather_start(a, buf):
        for k in range(1, X):
            launch(
                remote(
                    buf.at[t],
                    buf.at[t],
                    ag_send.at[a, k],
                    ag_recv.at[a, t],
                    "tp",
                    tp_at(k) * 2 + c,
                )
            )
        launch(remote(buf.at[t], buf.at[t], ag_send.at[a, 0], ag_recv.at[a, t], "tp", peer))

    def gather_wait(a, buf, slot):
        remote(
            buf.at[slot], buf.at[slot], ag_send.at[a, 0], ag_recv.at[a, slot], "tp", peer
        ).wait_recv()

    def gather_forward(a, buf):
        for k in range(1, X):
            slot = tp_from(k) * 2 + c
            gather_wait(a, buf, slot)
            launch(
                remote(
                    buf.at[slot],
                    buf.at[slot],
                    ag_send.at[a, X - 1 + k],
                    ag_recv.at[a, slot],
                    "tp",
                    peer,
                )
            )

    def gather_finish(a, buf):
        gather_forward(a, buf)
        for k in range(X):
            gather_wait(a, buf, tp_from(k) * 2 + other)

    def project_source(layer, at):
        rows = xs[pl.ds(2 * at, 2)].reshape(2 * Rs, D)

        def one(j, carry):
            kv[j, at] = mm(rows, wkv[j]).astype(BF)
            return carry

        lax.fori_loop(2 * layer, 2 * layer + 2, one, 0)

    def send_queries(layer):
        load_q[layer].wait()
        rows = xt[layer].reshape(T, D)
        qall[layer, s] = mm(rows, wq[layer]).astype(BF)
        for i in range(1, S):
            launch(
                remote(
                    qall.at[layer, s],
                    qall.at[layer, s],
                    q_send.at[layer, i],
                    q_recv.at[layer, s],
                    "sp",
                    sp_at(i),
                )
            )

    def attend_block(layer, block, sums, stats):
        lanes = lax.broadcasted_iota(jnp.int32, (T, LANES), 1)
        packed = jnp.zeros((T, LANES), F32)
        for h in range(heads):
            cols = slice(h * HD, (h + 1) * HD)
            query = qall[layer, block, :, cols]
            keys = kv[2 * layer, :, :, cols].reshape(n * Rs, HD)
            values = kv[2 * layer + 1, :, :, cols].reshape(n * Rs, HD)
            scores = (
                lax.dot_general(query, keys, (((1,), (1,)), ((), ())), preferred_element_type=F32)
                * scale
            )
            top = jnp.max(scores, axis=-1, keepdims=True)
            raised = jnp.exp(scores - top)
            total = jnp.sum(raised, axis=-1, keepdims=True)
            sums[:, cols] = mm(raised.astype(BF), values).astype(BF)
            packed = jnp.where(lanes == 2 * h, top, packed)
            packed = jnp.where(lanes == 2 * h + 1, total, packed)
        stats[...] = packed.T[:STAT_ROWS]

    def sums_copy(layer, i, slot, block):
        return remote(
            osend.at[layer, i],
            orecv.at[layer, slot],
            r_send.at[layer, i],
            r_recv.at[layer, slot],
            "sp",
            block,
        )

    def stats_copy(layer, i, slot, block):
        return remote(
            ssend.at[layer, i],
            srecv.at[layer, slot],
            s_send.at[layer, i],
            s_recv.at[layer, slot],
            "sp",
            block,
        )

    def attend(layer, meanwhile):
        attend_block(layer, s, orecv.at[layer, s], srecv.at[layer, s])

        def one(i, carry):
            block = sp_at(i)
            remote(
                qall.at[layer, block],
                qall.at[layer, block],
                q_send.at[layer, 0],
                q_recv.at[layer, block],
                "sp",
                block,
            ).wait_recv()
            attend_block(layer, block, osend.at[layer, i], ssend.at[layer, i])
            sums_copy(layer, i, s, block).start()
            stats_copy(layer, i, s, block).start()
            return carry

        lax.fori_loop(1, S, one, 0)
        meanwhile()
        for i in range(1, S):
            block = sp_at(i)
            pending.append(sums_copy(layer, i, s, block))
            pending.append(stats_copy(layer, i, s, block))
            sums_copy(layer, i, block, block).wait_recv()
            stats_copy(layer, i, block, block).wait_recv()
        rows = srecv[layer].reshape(S * STAT_ROWS, T)
        if S * STAT_ROWS < LANES:
            rows = jnp.concatenate([rows, jnp.zeros((LANES - S * STAT_ROWS, T), F32)], axis=0)
        stats = rows.T
        for h in range(heads):
            cols = slice(h * HD, (h + 1) * HD)
            tops = [stats[:, b * STAT_ROWS + 2 * h :][:, :1] for b in range(S)]
            highest = functools.reduce(jnp.maximum, tops)
            total = jnp.zeros((T, 1), F32)
            summed = jnp.zeros((T, HD), F32)
            for b in range(S):
                factor = jnp.exp(tops[b] - highest)
                total = total + factor * stats[:, b * STAT_ROWS + 2 * h + 1 :][:, :1]
                summed = summed + factor * orecv[layer, b, :, cols].astype(F32)
            att[:, cols] = (summed / total).astype(BF)
        load_o[layer].wait()
        spread_sum(layer, att, wo.at[layer])

    def spread_sum(a, lhs, weight):
        def one(j, carry):
            cols = pl.ds(pl.multiple_of(j * TILE, TILE), TILE)
            pf[:, :, cols] = mm(lhs[...], weight[:, cols]).reshape(n, Rt, TILE)
            return carry

        lax.fori_loop(0, D // TILE, one, 0)
        order = [*range(1, X), 0]

        def first(k):
            return remote(
                p1s.at[a, k], p1r.at[a, k], p1_send.at[a, k], p1_recv.at[a, k], "tp", peer
            )

        def second(k):
            return remote(
                p2s.at[a, k],
                p2r.at[a, k],
                p2_send.at[a, k],
                p2_recv.at[a, k],
                "tp",
                tp_at(k) * 2 + c,
            )

        for k in order:
            p1s[a, k] = pf[tp_at(k) * 2 + other].astype(BF)
            launch(first(k))
        for k in range(1, X):
            first(k).wait_recv()
            p2s[a, k] = (pf[tp_at(k) * 2 + c] + p1r[a, k].astype(F32)).astype(BF)
            launch(second(k))
        first(0).wait_recv()
        own = pf[t] + p1r[a, 0].astype(F32)
        for k in range(1, X):
            second(k).wait_recv()
            own = own + p2r[a, k].astype(F32)
        residual[...] = residual[...] + own

    load_t.wait()
    residual[...] = tv[...].astype(F32)
    xt[0, t] = normed_rows(residual[...], attend_gain[0:1]).astype(BF)
    pl.semaphore_wait(barrier, X + S - 1)
    gather_start(0, xt.at[0])
    load_s.wait()
    step = 32

    def norm_source(j, carry):
        rows = pl.ds(pl.multiple_of(j * step, step), step)
        xs[t, rows] = normed_rows(sv[rows].astype(F32), source_gain[...]).astype(BF)
        return carry

    lax.fori_loop(0, Rs // step, norm_source, 0)
    gather_start(3, xs)
    gather_finish(0, xt.at[0])
    send_queries(0)
    for copy in load_kv[0]:
        copy.wait()
    gather_wait(3, xs, peer)
    project_source(0, x)
    for copy in load_kv[1]:
        copy.wait()
    project_source(1, x)
    gather_forward(3, xs)
    for k in range(1, X):
        gather_wait(3, xs, tp_from(k) * 2 + other)
        project_source(0, tp_from(k))

    def rest_of_source():
        for k in range(1, X):
            project_source(1, tp_from(k))

    attend(0, rest_of_source)
    xt[1, t] = normed_rows(residual[...], attend_gain[1:2]).astype(BF)
    gather_start(1, xt.at[1])
    gather_finish(1, xt.at[1])
    send_queries(1)
    attend(1, lambda: None)
    xt[2, t] = normed_rows(residual[...], mixer_gain[...]).astype(BF)
    gather_start(2, xt.at[2])
    gather_finish(2, xt.at[2])
    load_m[0].wait()
    load_m[1].wait()
    mixed = xt[2].reshape(T, D)
    for pad, weight, number in ((gpad, wg, 0), (upad, wu, 1)):
        lifted = mm(mixed, weight[...]).astype(BF).astype(F32)
        pad[8:] = lifted
        hs[number] = lifted[T - 8 :]
    halo_out = remote(hs, hr, h_send, h_recv, "sp", lax.rem(s + 1, S))

    @pl.when(s < S - 1)
    def _():
        halo_out.start()

    @pl.when(s == 0)
    def _():
        gpad[:8] = jnp.zeros((8, F), F32)
        upad[:8] = jnp.zeros((8, F), F32)

    @pl.when(s > 0)
    def _():
        halo_out.wait_recv()
        gpad[:8] = hr[0]
        upad[:8] = hr[1]

    @pl.when(s < S - 1)
    def _():
        halo_out.wait_send()

    def convolved(pad, taps):
        return (
            taps[0:1] * pad[6 : 6 + T] + taps[1:2] * pad[7 : 7 + T] + taps[2:3] * pad[8 : 8 + T]
        )

    gate = convolved(gpad, gate_taps)
    hid[...] = (gate / (1.0 + jnp.exp(-gate)) * convolved(upad, up_taps)).astype(BF)
    load_m[2].wait()
    spread_sum(2, hid, wd)
    result[...] = normed_rows(residual[...], final_gain[...]).astype(BF)
    for copy in pending:
        copy.wait_send()


def body(n, S, *arrays):
    (
        source,
        target,
        source_gain,
        attend_gain,
        query_weight,
        key_weight,
        value_weight,
        out_weight,
        mixer_gain,
        gate_weight,
        up_weight,
        gate_taps,
        up_taps,
        down_weight,
        final_gain,
    ) = arrays
    Rs, D = source.shape
    Rt = target.shape[0]
    W = query_weight.shape[2]
    F = gate_weight.shape[1]
    T = n * Rt
    X = n // 2
    hbm = pl.BlockSpec(memory_space=pl.ANY)
    vmem = pl.BlockSpec(memory_space=pltpu.VMEM)
    dma = pltpu.SemaphoreType.DMA
    scratch = [
        pltpu.VMEM((Rs, D), BF),
        pltpu.VMEM((Rt, D), BF),
        pltpu.VMEM((2, D, W), BF),
        pltpu.VMEM((4, D, W), BF),
        pltpu.VMEM((2, W, D), BF),
        pltpu.VMEM((D, F), BF),
        pltpu.VMEM((D, F), BF),
        pltpu.VMEM((F, D), BF),
        pltpu.VMEM((n, Rs, D), BF),
        pltpu.VMEM((3, n, Rt, D), BF),
        pltpu.VMEM((4, X, 2 * Rs, W), BF),
        pltpu.VMEM((2, S, T, W), BF),
        pltpu.VMEM((2, S, T, W), BF),
        pltpu.VMEM((2, S, T, W), BF),
        pltpu.VMEM((2, S, STAT_ROWS, T), F32),
        pltpu.VMEM((2, S, STAT_ROWS, T), F32),
        pltpu.VMEM((n, Rt, D), F32),
        pltpu.VMEM((T, W), BF),
        pltpu.VMEM((3, X, Rt, D), BF),
        pltpu.VMEM((3, X, Rt, D), BF),
        pltpu.VMEM((3, X, Rt, D), BF),
        pltpu.VMEM((3, X, Rt, D), BF),
        pltpu.VMEM((2, 8, F), F32),
        pltpu.VMEM((2, 8, F), F32),
        pltpu.VMEM((T + 8, F), F32),
        pltpu.VMEM((T + 8, F), F32),
        pltpu.VMEM((T, F), BF),
        pltpu.VMEM((Rt, D), F32),
        dma((2,)),
        dma((11,)),
        dma((4, n)),
        dma((4, n)),
        dma((2, S)),
        dma((2, S)),
        dma((2, S)),
        dma((2, S)),
        dma((2, S)),
        dma((2, S)),
        dma((3, X)),
        dma((3, X)),
        dma((3, X)),
        dma((3, X)),
        dma,
        dma,
    ]
    return pl.pallas_call(
        functools.partial(kernel, n, S),
        out_shape=jax.ShapeDtypeStruct((Rt, D), BF),
        in_specs=[
            hbm,
            hbm,
            vmem,
            vmem,
            hbm,
            hbm,
            hbm,
            hbm,
            vmem,
            hbm,
            hbm,
            vmem,
            vmem,
            hbm,
            vmem,
        ],
        out_specs=vmem,
        scratch_shapes=scratch,
        compiler_params=pltpu.CompilerParams(
            collective_id=0, has_side_effects=True, vmem_limit_bytes=67043328
        ),
    )(
        source,
        target,
        source_gain.reshape(1, D),
        attend_gain,
        query_weight,
        key_weight,
        value_weight,
        out_weight,
        mixer_gain.reshape(1, D),
        gate_weight,
        up_weight,
        gate_taps,
        up_taps,
        down_weight,
        final_gain.reshape(1, D),
    )


def solution(mesh):
    placed = (
        P(("grp", "sp", "tp"), None),
        P(("grp", "sp", "tp"), None),
        P(),
        P(),
        P(None, None, "tp"),
        P(None, None, "tp"),
        P(None, None, "tp"),
        P(None, "tp", None),
        P(),
        P(None, "tp"),
        P(None, "tp"),
        P(None, "tp"),
        P(None, "tp"),
        P("tp", None),
        P(),
    )
    return jax.shard_map(
        functools.partial(body, mesh.shape["tp"], mesh.shape["sp"]),
        mesh=mesh,
        in_specs=placed,
        out_specs=P(("grp", "sp", "tp"), None),
        check_vma=False,
    )
```

```python
import functools

import jax
import jax.numpy as jnp
from jax import lax
from jax.experimental import pallas as pl
from jax.experimental.pallas import tpu as pltpu
from jax.sharding import PartitionSpec as P

HD = 256
EPS = 1e-06
TILE = 256
STAT_ROWS = 8
LANES = 128
MESH = pl.DeviceIdType.MESH
BF = jnp.bfloat16
F32 = jnp.float32


def normed_rows(wide, gain):
    return wide * lax.rsqrt(jnp.mean(wide * wide, axis=-1, keepdims=True) + EPS) * gain


def mm(a, b):
    return jnp.dot(a, b, preferred_element_type=F32)


def kernel(
    n,
    S,
    source,
    target,
    source_gain,
    attend_gain,
    query_weight,
    key_weight,
    value_weight,
    out_weight,
    mixer_gain,
    gate_weight,
    up_weight,
    gate_taps,
    up_taps,
    down_weight,
    final_gain,
    result,
    sv,
    tv,
    wq,
    wkv,
    wo,
    wg,
    wu,
    wd,
    xs,
    xt,
    kv,
    qall,
    osend,
    orecv,
    ssend,
    srecv,
    pf,
    att,
    p1s,
    p1r,
    p2s,
    p2r,
    hs,
    hr,
    gpad,
    upad,
    hid,
    residual,
    load_sem,
    w_sem,
    ag_send,
    ag_recv,
    q_send,
    q_recv,
    r_send,
    r_recv,
    s_send,
    s_recv,
    p1_send,
    p1_recv,
    p2_send,
    p2_recv,
    h_send,
    h_recv,
):
    X = n // 2
    Rs, D = source.shape
    Rt = target.shape[0]
    W = wq.shape[2]
    T = n * Rt
    heads = W // HD
    F = wg.shape[0]
    scale = HD ** (-0.5)
    t = lax.axis_index("tp")
    s = lax.axis_index("sp")
    x = lax.div(t, 2)
    c = lax.rem(t, 2)
    other = 1 - c
    peer = x * 2 + other
    pending = []

    def tp_at(k):
        return lax.rem(x + k, X)

    def tp_from(k):
        return lax.rem(x + X - k, X)

    def sp_at(i):
        return lax.rem(s + i, S)

    def remote(src, dst, ss, rs, axis, where):
        return pltpu.make_async_remote_copy(
            src_ref=src,
            dst_ref=dst,
            send_sem=ss,
            recv_sem=rs,
            device_id={axis: where},
            device_id_type=MESH,
        )

    def launch(copy):
        copy.start()
        pending.append(copy)

    barrier = pltpu.get_barrier_semaphore()
    pl.semaphore_signal(barrier, inc=1, device_id={"tp": peer}, device_id_type=MESH)
    for k in range(1, X):
        pl.semaphore_signal(
            barrier, inc=1, device_id={"tp": tp_at(k) * 2 + c}, device_id_type=MESH
        )
    for i in range(1, S):
        pl.semaphore_signal(barrier, inc=1, device_id={"sp": sp_at(i)}, device_id_type=MESH)

    load_t = pltpu.make_async_copy(target, tv, load_sem.at[0])
    load_s = pltpu.make_async_copy(source, sv, load_sem.at[1])
    load_t.start()
    load_s.start()
    load_q = [pltpu.make_async_copy(query_weight.at[l], wq.at[l], w_sem.at[l]) for l in range(2)]
    load_kv = []
    for l in range(2):
        load_kv.append(
            [
                pltpu.make_async_copy(key_weight.at[l], wkv.at[2 * l], w_sem.at[2 + 2 * l]),
                pltpu.make_async_copy(value_weight.at[l], wkv.at[2 * l + 1], w_sem.at[3 + 2 * l]),
            ]
        )
    load_o = [pltpu.make_async_copy(out_weight.at[l], wo.at[l], w_sem.at[6 + l]) for l in range(2)]
    load_m = [
        pltpu.make_async_copy(gate_weight, wg, w_sem.at[8]),
        pltpu.make_async_copy(up_weight, wu, w_sem.at[9]),
        pltpu.make_async_copy(down_weight, wd, w_sem.at[10]),
    ]
    for copy in [load_q[0], *load_kv[0], *load_kv[1], load_o[0], load_q[1], load_o[1], *load_m]:
        copy.start()

    def gather_start(a, buf):
        for k in range(1, X):
            launch(
                remote(
                    buf.at[t],
                    buf.at[t],
                    ag_send.at[a, k],
                    ag_recv.at[a, t],
                    "tp",
                    tp_at(k) * 2 + c,
                )
            )
        launch(remote(buf.at[t], buf.at[t], ag_send.at[a, 0], ag_recv.at[a, t], "tp", peer))

    def gather_wait(a, buf, slot):
        remote(
            buf.at[slot], buf.at[slot], ag_send.at[a, 0], ag_recv.at[a, slot], "tp", peer
        ).wait_recv()

    def gather_forward(a, buf):
        for k in range(1, X):
            slot = tp_from(k) * 2 + c
            gather_wait(a, buf, slot)
            launch(
                remote(
                    buf.at[slot],
                    buf.at[slot],
                    ag_send.at[a, X - 1 + k],
                    ag_recv.at[a, slot],
                    "tp",
                    peer,
                )
            )

    def gather_finish(a, buf):
        gather_forward(a, buf)
        for k in range(X):
            gather_wait(a, buf, tp_from(k) * 2 + other)

    def project_source(layer, at):
        rows = xs[pl.ds(2 * at, 2)].reshape(2 * Rs, D)

        def one(j, carry):
            kv[j, at] = mm(rows, wkv[j]).astype(BF)
            return carry

        lax.fori_loop(2 * layer, 2 * layer + 2, one, 0)

    def has_next(way, where):
        return where < S - 1 if way == 0 else where > 0

    def query_copy(layer, way, block):
        return remote(
            qall.at[layer, block],
            qall.at[layer, block],
            q_send.at[layer, way, block],
            q_recv.at[layer, block],
            "sp",
            jnp.clip(s + 1 - 2 * way, 0, S - 1),
        )

    def send_queries(layer):
        load_q[layer].wait()
        rows = xt[layer].reshape(T, D)
        qall[layer, s] = mm(rows, wq[layer]).astype(BF)
        for way in range(2):

            @pl.when(has_next(way, s))
            def _():
                query_copy(layer, way, s).start()

    def attend_block(layer, block, sums, stats):
        lanes = lax.broadcasted_iota(jnp.int32, (T, LANES), 1)
        packed = jnp.zeros((T, LANES), F32)
        for h in range(heads):
            cols = slice(h * HD, (h + 1) * HD)
            query = qall[layer, block, :, cols]
            keys = kv[2 * layer, :, :, cols].reshape(n * Rs, HD)
            values = kv[2 * layer + 1, :, :, cols].reshape(n * Rs, HD)
            scores = (
                lax.dot_general(query, keys, (((1,), (1,)), ((), ())), preferred_element_type=F32)
                * scale
            )
            top = jnp.max(scores, axis=-1, keepdims=True)
            raised = jnp.exp(scores - top)
            total = jnp.sum(raised, axis=-1, keepdims=True)
            sums[:, cols] = mm(raised.astype(BF), values).astype(BF)
            packed = jnp.where(lanes == 2 * h, top, packed)
            packed = jnp.where(lanes == 2 * h + 1, total, packed)
        stats[...] = packed.T[:STAT_ROWS]

    def sums_copy(layer, i, slot, block):
        return remote(
            osend.at[layer, i],
            orecv.at[layer, slot],
            r_send.at[layer, i],
            r_recv.at[layer, slot],
            "sp",
            block,
        )

    def stats_copy(layer, i, slot, block):
        return remote(
            ssend.at[layer, i],
            srecv.at[layer, slot],
            s_send.at[layer, i],
            s_recv.at[layer, slot],
            "sp",
            block,
        )

    def attend(layer, meanwhile):
        attend_block(layer, s, orecv.at[layer, s], srecv.at[layer, s])

        def one(i, carry):
            for way in range(2):
                block = s - i if way == 0 else s + i

                @pl.when(block >= 0 if way == 0 else block < S)
                def _():
                    query_copy(layer, way, block).wait_recv()

                    @pl.when(has_next(way, s))
                    def _():
                        query_copy(layer, way, block).start()

            for way in range(2):
                block = s - i if way == 0 else s + i

                @pl.when(block >= 0 if way == 0 else block < S)
                def _():
                    attend_block(layer, block, osend.at[layer, block], ssend.at[layer, block])
                    sums_copy(layer, block, s, block).start()
                    stats_copy(layer, block, s, block).start()

            return carry

        lax.fori_loop(1, S, one, 0)
        meanwhile()

        def wait_block(i, carry):
            block = sp_at(i)
            sums_copy(layer, block, block, block).wait_recv()
            stats_copy(layer, block, block, block).wait_recv()
            return carry

        lax.fori_loop(1, S, wait_block, 0)
        rows = srecv[layer].reshape(S * STAT_ROWS, T)
        if S * STAT_ROWS < LANES:
            rows = jnp.concatenate([rows, jnp.zeros((LANES - S * STAT_ROWS, T), F32)], axis=0)
        stats = rows.T
        for h in range(heads):
            cols = slice(h * HD, (h + 1) * HD)
            tops = [stats[:, b * STAT_ROWS + 2 * h :][:, :1] for b in range(S)]
            highest = functools.reduce(jnp.maximum, tops)
            total = jnp.zeros((T, 1), F32)
            summed = jnp.zeros((T, HD), F32)
            for b in range(S):
                factor = jnp.exp(tops[b] - highest)
                total = total + factor * stats[:, b * STAT_ROWS + 2 * h + 1 :][:, :1]
                summed = summed + factor * orecv[layer, b, :, cols].astype(F32)
            att[:, cols] = (summed / total).astype(BF)
        load_o[layer].wait()
        spread_sum(layer, att, wo.at[layer])

    def spread_sum(a, lhs, weight):
        def one(j, carry):
            cols = pl.ds(pl.multiple_of(j * TILE, TILE), TILE)
            pf[:, :, cols] = mm(lhs[...], weight[:, cols]).reshape(n, Rt, TILE)
            return carry

        lax.fori_loop(0, D // TILE, one, 0)
        order = [*range(1, X), 0]

        def first(k):
            return remote(
                p1s.at[a, k], p1r.at[a, k], p1_send.at[a, k], p1_recv.at[a, k], "tp", peer
            )

        def second(k):
            return remote(
                p2s.at[a, k],
                p2r.at[a, k],
                p2_send.at[a, k],
                p2_recv.at[a, k],
                "tp",
                tp_at(k) * 2 + c,
            )

        for k in order:
            p1s[a, k] = pf[tp_at(k) * 2 + other].astype(BF)
            launch(first(k))
        for k in range(1, X):
            first(k).wait_recv()
            p2s[a, k] = (pf[tp_at(k) * 2 + c] + p1r[a, k].astype(F32)).astype(BF)
            launch(second(k))
        first(0).wait_recv()
        own = pf[t] + p1r[a, 0].astype(F32)
        for k in range(1, X):
            second(k).wait_recv()
            own = own + p2r[a, k].astype(F32)
        residual[...] = residual[...] + own

    load_t.wait()
    residual[...] = tv[...].astype(F32)
    xt[0, t] = normed_rows(residual[...], attend_gain[0:1]).astype(BF)
    pl.semaphore_wait(barrier, X + S - 1)
    gather_start(0, xt.at[0])
    load_s.wait()
    step = 32

    def norm_source(j, carry):
        rows = pl.ds(pl.multiple_of(j * step, step), step)
        xs[t, rows] = normed_rows(sv[rows].astype(F32), source_gain[...]).astype(BF)
        return carry

    lax.fori_loop(0, Rs // step, norm_source, 0)
    gather_start(3, xs)
    gather_finish(0, xt.at[0])
    send_queries(0)
    for copy in load_kv[0]:
        copy.wait()
    gather_wait(3, xs, peer)
    project_source(0, x)
    for copy in load_kv[1]:
        copy.wait()
    project_source(1, x)
    gather_forward(3, xs)
    for k in range(1, X):
        gather_wait(3, xs, tp_from(k) * 2 + other)
        project_source(0, tp_from(k))

    def rest_of_source():
        for k in range(1, X):
            project_source(1, tp_from(k))

    attend(0, rest_of_source)
    xt[1, t] = normed_rows(residual[...], attend_gain[1:2]).astype(BF)
    gather_start(1, xt.at[1])
    gather_finish(1, xt.at[1])
    send_queries(1)
    attend(1, lambda: None)
    xt[2, t] = normed_rows(residual[...], mixer_gain[...]).astype(BF)
    gather_start(2, xt.at[2])
    gather_finish(2, xt.at[2])
    load_m[0].wait()
    load_m[1].wait()
    mixed = xt[2].reshape(T, D)
    for pad, weight, number in ((gpad, wg, 0), (upad, wu, 1)):
        lifted = (
            lax.dot_general(
                mixed, weight[...], (((1,), (1,)), ((), ())), preferred_element_type=F32
            )
            .astype(BF)
            .astype(F32)
        )
        pad[8:] = lifted
        hs[number] = lifted[T - 8 :]
    halo_out = remote(hs, hr, h_send, h_recv, "sp", lax.rem(s + 1, S))

    @pl.when(s < S - 1)
    def _():
        halo_out.start()

    @pl.when(s == 0)
    def _():
        gpad[:8] = jnp.zeros((8, F), F32)
        upad[:8] = jnp.zeros((8, F), F32)

    @pl.when(s > 0)
    def _():
        halo_out.wait_recv()
        gpad[:8] = hr[0]
        upad[:8] = hr[1]

    @pl.when(s < S - 1)
    def _():
        halo_out.wait_send()

    def convolved(pad, taps):
        return (
            taps[0:1] * pad[6 : 6 + T] + taps[1:2] * pad[7 : 7 + T] + taps[2:3] * pad[8 : 8 + T]
        )

    gate = convolved(gpad, gate_taps)
    hid[...] = (gate / (1.0 + jnp.exp(-gate)) * convolved(upad, up_taps)).astype(BF)
    load_m[2].wait()
    spread_sum(2, hid, wd)
    result[...] = normed_rows(residual[...], final_gain[...]).astype(BF)
    for copy in pending:
        copy.wait_send()
    for layer in range(2):

        def wait_sent(block, carry):
            for way in range(2):

                @pl.when(has_next(way, s) & (block <= s if way == 0 else block >= s))
                def _():
                    query_copy(layer, way, block).wait_send()

            @pl.when(block != s)
            def _():
                sums_copy(layer, block, s, block).wait_send()
                stats_copy(layer, block, s, block).wait_send()

            return carry

        lax.fori_loop(0, S, wait_sent, 0)


def body(n, S, *arrays):
    (
        source,
        target,
        source_gain,
        attend_gain,
        query_weight,
        key_weight,
        value_weight,
        out_weight,
        mixer_gain,
        gate_weight,
        up_weight,
        gate_taps,
        up_taps,
        down_weight,
        final_gain,
    ) = arrays
    Rs, D = source.shape
    Rt = target.shape[0]
    W = query_weight.shape[2]
    F = gate_weight.shape[1]
    T = n * Rt
    X = n // 2
    hbm = pl.BlockSpec(memory_space=pl.ANY)
    vmem = pl.BlockSpec(memory_space=pltpu.VMEM)
    dma = pltpu.SemaphoreType.DMA
    scratch = [
        pltpu.VMEM((Rs, D), BF),
        pltpu.VMEM((Rt, D), BF),
        pltpu.VMEM((2, D, W), BF),
        pltpu.VMEM((4, D, W), BF),
        pltpu.VMEM((2, W, D), BF),
        pltpu.VMEM((F, D), BF),
        pltpu.VMEM((F, D), BF),
        pltpu.VMEM((F, D), BF),
        pltpu.VMEM((n, Rs, D), BF),
        pltpu.VMEM((3, n, Rt, D), BF),
        pltpu.VMEM((4, X, 2 * Rs, W), BF),
        pltpu.VMEM((2, S, T, W), BF),
        pltpu.VMEM((2, S, T, W), BF),
        pltpu.VMEM((2, S, T, W), BF),
        pltpu.VMEM((2, S, STAT_ROWS, T), F32),
        pltpu.VMEM((2, S, STAT_ROWS, T), F32),
        pltpu.VMEM((n, Rt, D), F32),
        pltpu.VMEM((T, W), BF),
        pltpu.VMEM((3, X, Rt, D), BF),
        pltpu.VMEM((3, X, Rt, D), BF),
        pltpu.VMEM((3, X, Rt, D), BF),
        pltpu.VMEM((3, X, Rt, D), BF),
        pltpu.VMEM((2, 8, F), F32),
        pltpu.VMEM((2, 8, F), F32),
        pltpu.VMEM((T + 8, F), F32),
        pltpu.VMEM((T + 8, F), F32),
        pltpu.VMEM((T, F), BF),
        pltpu.VMEM((Rt, D), F32),
        dma((2,)),
        dma((11,)),
        dma((4, n)),
        dma((4, n)),
        dma((2, 2, S)),
        dma((2, S)),
        dma((2, S)),
        dma((2, S)),
        dma((2, S)),
        dma((2, S)),
        dma((3, X)),
        dma((3, X)),
        dma((3, X)),
        dma((3, X)),
        dma,
        dma,
    ]
    return pl.pallas_call(
        functools.partial(kernel, n, S),
        out_shape=jax.ShapeDtypeStruct((Rt, D), BF),
        in_specs=[
            hbm,
            hbm,
            vmem,
            vmem,
            hbm,
            hbm,
            hbm,
            hbm,
            vmem,
            hbm,
            hbm,
            vmem,
            vmem,
            hbm,
            vmem,
        ],
        out_specs=vmem,
        scratch_shapes=scratch,
        compiler_params=pltpu.CompilerParams(
            collective_id=0, has_side_effects=True, vmem_limit_bytes=67043328
        ),
    )(
        source,
        target,
        source_gain.reshape(1, D),
        attend_gain,
        query_weight,
        key_weight,
        value_weight,
        out_weight,
        mixer_gain.reshape(1, D),
        gate_weight.T,
        up_weight.T,
        gate_taps,
        up_taps,
        down_weight,
        final_gain.reshape(1, D),
    )


def solution(mesh):
    placed = (
        P(("grp", "sp", "tp"), None),
        P(("grp", "sp", "tp"), None),
        P(),
        P(),
        P(None, None, "tp"),
        P(None, None, "tp"),
        P(None, None, "tp"),
        P(None, "tp", None),
        P(),
        P(None, "tp"),
        P(None, "tp"),
        P(None, "tp"),
        P(None, "tp"),
        P("tp", None),
        P(),
    )
    return jax.shard_map(
        functools.partial(body, mesh.shape["tp"], mesh.shape["sp"]),
        mesh=mesh,
        in_specs=placed,
        out_specs=P(("grp", "sp", "tp"), None),
        check_vma=False,
    )
```

```python
import functools

import jax
import jax.numpy as jnp
from jax import lax
from jax.experimental import pallas as pl
from jax.experimental.pallas import tpu as pltpu
from jax.sharding import PartitionSpec as P

HD = 256
EPS = 1e-06
TILE = 256
STAT_ROWS = 8
LANES = 128
MESH = pl.DeviceIdType.MESH
BF = jnp.bfloat16
F32 = jnp.float32


def normed_rows(wide, gain):
    return wide * lax.rsqrt(jnp.mean(wide * wide, axis=-1, keepdims=True) + EPS) * gain


def mm(a, b):
    return jnp.dot(a, b, preferred_element_type=F32)


def kernel(
    n,
    S,
    source,
    target,
    source_gain,
    attend_gain,
    query_weight,
    key_weight,
    value_weight,
    out_weight,
    mixer_gain,
    gate_weight,
    up_weight,
    gate_taps,
    up_taps,
    down_weight,
    final_gain,
    result,
    sv,
    tv,
    wq,
    wkv,
    wo,
    wg,
    wu,
    wd,
    xs,
    xt,
    kv,
    qall,
    osend,
    orecv,
    ssend,
    srecv,
    pf,
    att,
    p1s,
    p1r,
    p2s,
    p2r,
    hs,
    hr,
    gpad,
    upad,
    hid,
    residual,
    load_sem,
    w_sem,
    ag_send,
    ag_recv,
    q_send,
    q_recv,
    r_send,
    r_recv,
    s_send,
    s_recv,
    p1_send,
    p1_recv,
    p2_send,
    p2_recv,
    h_send,
    h_recv,
):
    X = n // 2
    Rs, D = source.shape
    Rt = target.shape[0]
    W = wq.shape[2]
    T = n * Rt
    heads = W // HD
    F = wg.shape[0]
    scale = HD ** (-0.5)
    t = lax.axis_index("tp")
    s = lax.axis_index("sp")
    x = lax.div(t, 2)
    c = lax.rem(t, 2)
    other = 1 - c
    peer = x * 2 + other
    pending = []

    def tp_at(k):
        return lax.rem(x + k, X)

    def tp_from(k):
        return lax.rem(x + X - k, X)

    def sp_at(i):
        return lax.rem(s + i, S)

    def remote(src, dst, ss, rs, axis, where):
        return pltpu.make_async_remote_copy(
            src_ref=src,
            dst_ref=dst,
            send_sem=ss,
            recv_sem=rs,
            device_id={axis: where},
            device_id_type=MESH,
        )

    def launch(copy):
        copy.start()
        pending.append(copy)

    barrier = pltpu.get_barrier_semaphore()
    pl.semaphore_signal(barrier, inc=1, device_id={"tp": peer}, device_id_type=MESH)
    for k in range(1, X):
        pl.semaphore_signal(
            barrier, inc=1, device_id={"tp": tp_at(k) * 2 + c}, device_id_type=MESH
        )
    for i in range(1, S):
        pl.semaphore_signal(barrier, inc=1, device_id={"sp": sp_at(i)}, device_id_type=MESH)

    load_t = pltpu.make_async_copy(target, tv, load_sem.at[0])
    load_s = pltpu.make_async_copy(source, sv, load_sem.at[1])
    load_t.start()
    load_s.start()
    load_q = [pltpu.make_async_copy(query_weight.at[l], wq.at[l], w_sem.at[l]) for l in range(2)]
    load_kv = []
    for l in range(2):
        load_kv.append(
            [
                pltpu.make_async_copy(key_weight.at[l], wkv.at[2 * l], w_sem.at[2 + 2 * l]),
                pltpu.make_async_copy(value_weight.at[l], wkv.at[2 * l + 1], w_sem.at[3 + 2 * l]),
            ]
        )
    load_o = [pltpu.make_async_copy(out_weight.at[l], wo.at[l], w_sem.at[6 + l]) for l in range(2)]
    load_m = [
        pltpu.make_async_copy(gate_weight, wg, w_sem.at[8]),
        pltpu.make_async_copy(up_weight, wu, w_sem.at[9]),
        pltpu.make_async_copy(down_weight, wd, w_sem.at[10]),
    ]
    load_q[0].start()

    def gather_start(a, buf):
        for k in range(1, X):
            launch(
                remote(
                    buf.at[t],
                    buf.at[t],
                    ag_send.at[a, k],
                    ag_recv.at[a, t],
                    "tp",
                    tp_at(k) * 2 + c,
                )
            )
        launch(remote(buf.at[t], buf.at[t], ag_send.at[a, 0], ag_recv.at[a, t], "tp", peer))

    def gather_wait(a, buf, slot):
        remote(
            buf.at[slot], buf.at[slot], ag_send.at[a, 0], ag_recv.at[a, slot], "tp", peer
        ).wait_recv()

    def gather_forward(a, buf):
        for k in range(1, X):
            slot = tp_from(k) * 2 + c
            gather_wait(a, buf, slot)
            launch(
                remote(
                    buf.at[slot],
                    buf.at[slot],
                    ag_send.at[a, X - 1 + k],
                    ag_recv.at[a, slot],
                    "tp",
                    peer,
                )
            )

    def gather_finish(a, buf):
        gather_forward(a, buf)
        for k in range(X):
            gather_wait(a, buf, tp_from(k) * 2 + other)

    def project_source(layer, at):
        rows = xs[pl.ds(2 * at, 2)].reshape(2 * Rs, D)

        def one(j, carry):
            kv[j, at] = mm(rows, wkv[j]).astype(BF)
            return carry

        lax.fori_loop(2 * layer, 2 * layer + 2, one, 0)

    def query_copy(layer, i, block, where):
        return remote(
            qall.at[layer, block],
            qall.at[layer, block],
            q_send.at[layer, i],
            q_recv.at[layer, block],
            "sp",
            where,
        )

    def send_queries(layer):
        load_q[layer].wait()
        rows = xt[layer].reshape(T, D)
        qall[layer, s] = mm(rows, wq[layer]).astype(BF)
        for i in range(1, S):
            launch(query_copy(layer, i, s, sp_at(i)))

    def attend_block(layer, block, sums, stats):
        lanes = lax.broadcasted_iota(jnp.int32, (T, LANES), 1)
        packed = jnp.zeros((T, LANES), F32)
        for h in range(heads):
            cols = slice(h * HD, (h + 1) * HD)
            query = qall[layer, block, :, cols]
            keys = kv[2 * layer, :, :, cols].reshape(n * Rs, HD)
            values = kv[2 * layer + 1, :, :, cols].reshape(n * Rs, HD)
            scores = (
                lax.dot_general(query, keys, (((1,), (1,)), ((), ())), preferred_element_type=F32)
                * scale
            )
            top = jnp.max(scores, axis=-1, keepdims=True)
            raised = jnp.exp(scores - top)
            total = jnp.sum(raised, axis=-1, keepdims=True)
            sums[:, cols] = mm(raised.astype(BF), values).astype(BF)
            packed = jnp.where(lanes == 2 * h, top, packed)
            packed = jnp.where(lanes == 2 * h + 1, total, packed)
        stats[...] = packed.T[:STAT_ROWS]

    def sums_copy(layer, i, slot, block):
        return remote(
            osend.at[layer, i],
            orecv.at[layer, slot],
            r_send.at[layer, i],
            r_recv.at[layer, slot],
            "sp",
            block,
        )

    def stats_copy(layer, i, slot, block):
        return remote(
            ssend.at[layer, i],
            srecv.at[layer, slot],
            s_send.at[layer, i],
            s_recv.at[layer, slot],
            "sp",
            block,
        )

    def attend(layer, meanwhile):
        attend_block(layer, s, orecv.at[layer, s], srecv.at[layer, s])

        def one(i, carry):
            block = sp_at(i)
            query_copy(layer, 0, block, block).wait_recv()
            attend_block(layer, block, osend.at[layer, block], ssend.at[layer, block])
            sums_copy(layer, block, s, block).start()
            stats_copy(layer, block, s, block).start()
            return carry

        lax.fori_loop(1, S, one, 0)
        meanwhile()

        def wait_block(i, carry):
            block = sp_at(i)
            sums_copy(layer, block, block, block).wait_recv()
            stats_copy(layer, block, block, block).wait_recv()
            return carry

        lax.fori_loop(1, S, wait_block, 0)
        rows = srecv[layer].reshape(S * STAT_ROWS, T)
        if S * STAT_ROWS < LANES:
            rows = jnp.concatenate([rows, jnp.zeros((LANES - S * STAT_ROWS, T), F32)], axis=0)
        stats = rows.T
        for h in range(heads):
            cols = slice(h * HD, (h + 1) * HD)
            tops = [stats[:, b * STAT_ROWS + 2 * h :][:, :1] for b in range(S)]
            highest = functools.reduce(jnp.maximum, tops)
            total = jnp.zeros((T, 1), F32)
            summed = jnp.zeros((T, HD), F32)
            for b in range(S):
                factor = jnp.exp(tops[b] - highest)
                total = total + factor * stats[:, b * STAT_ROWS + 2 * h + 1 :][:, :1]
                summed = summed + factor * orecv[layer, b, :, cols].astype(F32)
            att[:, cols] = (summed / total).astype(BF)
        load_o[layer].wait()
        spread_sum(layer, att, wo.at[layer])

    def spread_sum(a, lhs, weight):
        def one(j, carry):
            cols = pl.ds(pl.multiple_of(j * TILE, TILE), TILE)
            pf[:, :, cols] = mm(lhs[...], weight[:, cols]).reshape(n, Rt, TILE)
            return carry

        lax.fori_loop(0, D // TILE, one, 0)
        order = [*range(1, X), 0]

        def first(k):
            return remote(
                p1s.at[a, k], p1r.at[a, k], p1_send.at[a, k], p1_recv.at[a, k], "tp", peer
            )

        def second(k):
            return remote(
                p2s.at[a, k],
                p2r.at[a, k],
                p2_send.at[a, k],
                p2_recv.at[a, k],
                "tp",
                tp_at(k) * 2 + c,
            )

        for k in order:
            p1s[a, k] = pf[tp_at(k) * 2 + other].astype(BF)
            launch(first(k))
        for k in range(1, X):
            first(k).wait_recv()
            p2s[a, k] = (pf[tp_at(k) * 2 + c] + p1r[a, k].astype(F32)).astype(BF)
            launch(second(k))
        first(0).wait_recv()
        own = pf[t] + p1r[a, 0].astype(F32)
        for k in range(1, X):
            second(k).wait_recv()
            own = own + p2r[a, k].astype(F32)
        residual[...] = residual[...] + own

    load_t.wait()
    residual[...] = tv[...].astype(F32)
    xt[0, t] = normed_rows(residual[...], attend_gain[0:1]).astype(BF)
    pl.semaphore_wait(barrier, X + S - 1)
    gather_start(0, xt.at[0])
    for copy in load_kv[0]:
        copy.start()
    load_s.wait()
    step = 32

    def norm_source(j, carry):
        rows = pl.ds(pl.multiple_of(j * step, step), step)
        xs[t, rows] = normed_rows(sv[rows].astype(F32), source_gain[...]).astype(BF)
        return carry

    lax.fori_loop(0, Rs // step, norm_source, 0)
    gather_start(3, xs)
    gather_finish(0, xt.at[0])
    send_queries(0)
    for copy in [*load_kv[1], load_o[0], load_q[1], load_o[1]]:
        copy.start()
    for copy in load_kv[0]:
        copy.wait()
    gather_wait(3, xs, peer)
    project_source(0, x)
    for copy in load_kv[1]:
        copy.wait()
    project_source(1, x)
    for copy in load_m:
        copy.start()
    gather_forward(3, xs)
    for k in range(1, X):
        gather_wait(3, xs, tp_from(k) * 2 + other)
        project_source(0, tp_from(k))

    def rest_of_source():
        for k in range(1, X):
            project_source(1, tp_from(k))

    attend(0, rest_of_source)
    xt[1, t] = normed_rows(residual[...], attend_gain[1:2]).astype(BF)
    gather_start(1, xt.at[1])
    gather_finish(1, xt.at[1])
    send_queries(1)
    attend(1, lambda: None)
    xt[2, t] = normed_rows(residual[...], mixer_gain[...]).astype(BF)
    gather_start(2, xt.at[2])
    gather_finish(2, xt.at[2])
    load_m[0].wait()
    load_m[1].wait()
    mixed = xt[2].reshape(T, D)
    for pad, weight, number in ((gpad, wg, 0), (upad, wu, 1)):
        lifted = (
            lax.dot_general(
                mixed, weight[...], (((1,), (1,)), ((), ())), preferred_element_type=F32
            )
            .astype(BF)
            .astype(F32)
        )
        pad[8:] = lifted
        hs[number] = lifted[T - 8 :]
    halo_out = remote(hs, hr, h_send, h_recv, "sp", lax.rem(s + 1, S))

    @pl.when(s < S - 1)
    def _():
        halo_out.start()

    @pl.when(s == 0)
    def _():
        gpad[:8] = jnp.zeros((8, F), F32)
        upad[:8] = jnp.zeros((8, F), F32)

    @pl.when(s > 0)
    def _():
        halo_out.wait_recv()
        gpad[:8] = hr[0]
        upad[:8] = hr[1]

    @pl.when(s < S - 1)
    def _():
        halo_out.wait_send()

    def convolved(pad, taps):
        return (
            taps[0:1] * pad[6 : 6 + T] + taps[1:2] * pad[7 : 7 + T] + taps[2:3] * pad[8 : 8 + T]
        )

    gate = convolved(gpad, gate_taps)
    hid[...] = (gate / (1.0 + jnp.exp(-gate)) * convolved(upad, up_taps)).astype(BF)
    load_m[2].wait()
    spread_sum(2, hid, wd)
    result[...] = normed_rows(residual[...], final_gain[...]).astype(BF)
    for copy in pending:
        copy.wait_send()
    for layer in range(2):

        def wait_sent(i, carry):
            block = sp_at(i)
            sums_copy(layer, block, s, block).wait_send()
            stats_copy(layer, block, s, block).wait_send()
            return carry

        lax.fori_loop(1, S, wait_sent, 0)


def body(n, S, *arrays):
    (
        source,
        target,
        source_gain,
        attend_gain,
        query_weight,
        key_weight,
        value_weight,
        out_weight,
        mixer_gain,
        gate_weight,
        up_weight,
        gate_taps,
        up_taps,
        down_weight,
        final_gain,
    ) = arrays
    Rs, D = source.shape
    Rt = target.shape[0]
    W = query_weight.shape[2]
    F = gate_weight.shape[1]
    T = n * Rt
    X = n // 2
    hbm = pl.BlockSpec(memory_space=pl.ANY)
    vmem = pl.BlockSpec(memory_space=pltpu.VMEM)
    dma = pltpu.SemaphoreType.DMA
    scratch = [
        pltpu.VMEM((Rs, D), BF),
        pltpu.VMEM((Rt, D), BF),
        pltpu.VMEM((2, D, W), BF),
        pltpu.VMEM((4, D, W), BF),
        pltpu.VMEM((2, W, D), BF),
        pltpu.VMEM((F, D), BF),
        pltpu.VMEM((F, D), BF),
        pltpu.VMEM((F, D), BF),
        pltpu.VMEM((n, Rs, D), BF),
        pltpu.VMEM((3, n, Rt, D), BF),
        pltpu.VMEM((4, X, 2 * Rs, W), BF),
        pltpu.VMEM((2, S, T, W), BF),
        pltpu.VMEM((2, S, T, W), BF),
        pltpu.VMEM((2, S, T, W), BF),
        pltpu.VMEM((2, S, STAT_ROWS, T), F32),
        pltpu.VMEM((2, S, STAT_ROWS, T), F32),
        pltpu.VMEM((n, Rt, D), F32),
        pltpu.VMEM((T, W), BF),
        pltpu.VMEM((3, X, Rt, D), BF),
        pltpu.VMEM((3, X, Rt, D), BF),
        pltpu.VMEM((3, X, Rt, D), BF),
        pltpu.VMEM((3, X, Rt, D), BF),
        pltpu.VMEM((2, 8, F), F32),
        pltpu.VMEM((2, 8, F), F32),
        pltpu.VMEM((T + 8, F), F32),
        pltpu.VMEM((T + 8, F), F32),
        pltpu.VMEM((T, F), BF),
        pltpu.VMEM((Rt, D), F32),
        dma((2,)),
        dma((11,)),
        dma((4, n)),
        dma((4, n)),
        dma((2, S)),
        dma((2, S)),
        dma((2, S)),
        dma((2, S)),
        dma((2, S)),
        dma((2, S)),
        dma((3, X)),
        dma((3, X)),
        dma((3, X)),
        dma((3, X)),
        dma,
        dma,
    ]
    return pl.pallas_call(
        functools.partial(kernel, n, S),
        out_shape=jax.ShapeDtypeStruct((Rt, D), BF),
        in_specs=[
            hbm,
            hbm,
            vmem,
            vmem,
            hbm,
            hbm,
            hbm,
            hbm,
            vmem,
            hbm,
            hbm,
            vmem,
            vmem,
            hbm,
            vmem,
        ],
        out_specs=vmem,
        scratch_shapes=scratch,
        compiler_params=pltpu.CompilerParams(
            collective_id=0, has_side_effects=True, vmem_limit_bytes=67043328
        ),
    )(
        source,
        target,
        source_gain.reshape(1, D),
        attend_gain,
        query_weight,
        key_weight,
        value_weight,
        out_weight,
        mixer_gain.reshape(1, D),
        gate_weight.T,
        up_weight.T,
        gate_taps,
        up_taps,
        down_weight,
        final_gain.reshape(1, D),
    )


def solution(mesh):
    placed = (
        P(("grp", "sp", "tp"), None),
        P(("grp", "sp", "tp"), None),
        P(),
        P(),
        P(None, None, "tp"),
        P(None, None, "tp"),
        P(None, None, "tp"),
        P(None, "tp", None),
        P(),
        P(None, "tp"),
        P(None, "tp"),
        P(None, "tp"),
        P(None, "tp"),
        P("tp", None),
        P(),
    )
    return jax.shard_map(
        functools.partial(body, mesh.shape["tp"], mesh.shape["sp"]),
        mesh=mesh,
        in_specs=placed,
        out_specs=P(("grp", "sp", "tp"), None),
        check_vma=False,
    )
```

```python
import functools

import jax
import jax.numpy as jnp
from jax import lax
from jax.experimental import pallas as pl
from jax.experimental.pallas import tpu as pltpu
from jax.sharding import PartitionSpec as P

HD = 256
EPS = 1e-06
TILE = 256
STAT_ROWS = 8
LANES = 128
MESH = pl.DeviceIdType.MESH
BF = jnp.bfloat16
F32 = jnp.float32


def normed_rows(wide, gain):
    return wide * lax.rsqrt(jnp.mean(wide * wide, axis=-1, keepdims=True) + EPS) * gain


def mm(a, b):
    return jnp.dot(a, b, preferred_element_type=F32)


def kernel(
    n,
    S,
    source,
    target,
    source_gain,
    attend_gain,
    query_weight,
    key_weight,
    value_weight,
    out_weight,
    mixer_gain,
    gate_weight,
    up_weight,
    gate_taps,
    up_taps,
    down_weight,
    final_gain,
    result,
    sv,
    tv,
    wq,
    wkv,
    wo,
    wg,
    wu,
    wd,
    xs,
    xt,
    kv,
    qall,
    osend,
    orecv,
    ssend,
    srecv,
    pf,
    att,
    p1s,
    p1r,
    p2s,
    p2r,
    hs,
    hr,
    gpad,
    upad,
    hid,
    residual,
    load_sem,
    w_sem,
    ag_send,
    ag_recv,
    q_send,
    q_recv,
    r_send,
    r_recv,
    s_send,
    s_recv,
    p1_send,
    p1_recv,
    p2_send,
    p2_recv,
    h_send,
    h_recv,
):
    X = n // 2
    Rs, D = source.shape
    Rt = target.shape[0]
    W = wq.shape[2]
    T = n * Rt
    heads = W // HD
    F = wg.shape[0]
    scale = HD ** (-0.5)
    t = lax.axis_index("tp")
    s = lax.axis_index("sp")
    x = lax.div(t, 2)
    c = lax.rem(t, 2)
    other = 1 - c
    peer = x * 2 + other
    pending = []

    def tp_at(k):
        return lax.rem(x + k, X)

    def tp_from(k):
        return lax.rem(x + X - k, X)

    def sp_at(i):
        return lax.rem(s + i, S)

    def remote(src, dst, ss, rs, axis, where):
        return pltpu.make_async_remote_copy(
            src_ref=src,
            dst_ref=dst,
            send_sem=ss,
            recv_sem=rs,
            device_id={axis: where},
            device_id_type=MESH,
        )

    def launch(copy):
        copy.start()
        pending.append(copy)

    barrier = pltpu.get_barrier_semaphore()
    pl.semaphore_signal(barrier, inc=1, device_id={"tp": peer}, device_id_type=MESH)
    for k in range(1, X):
        pl.semaphore_signal(
            barrier, inc=1, device_id={"tp": tp_at(k) * 2 + c}, device_id_type=MESH
        )
    for i in range(1, S):
        pl.semaphore_signal(barrier, inc=1, device_id={"sp": sp_at(i)}, device_id_type=MESH)

    load_t = pltpu.make_async_copy(target, tv, load_sem.at[0])
    load_s = pltpu.make_async_copy(source, sv, load_sem.at[1])
    load_t.start()
    load_s.start()
    load_q = [pltpu.make_async_copy(query_weight.at[l], wq.at[l], w_sem.at[l]) for l in range(2)]
    load_kv = []
    for l in range(2):
        load_kv.append(
            [
                pltpu.make_async_copy(key_weight.at[l], wkv.at[2 * l], w_sem.at[2 + 2 * l]),
                pltpu.make_async_copy(value_weight.at[l], wkv.at[2 * l + 1], w_sem.at[3 + 2 * l]),
            ]
        )
    load_o = [pltpu.make_async_copy(out_weight.at[l], wo.at[l], w_sem.at[6 + l]) for l in range(2)]
    load_m = [
        pltpu.make_async_copy(gate_weight, wg, w_sem.at[8]),
        pltpu.make_async_copy(up_weight, wu, w_sem.at[9]),
        pltpu.make_async_copy(down_weight, wd, w_sem.at[10]),
    ]
    load_q[0].start()

    def gather_start(a, buf):
        for k in range(1, X):
            launch(
                remote(
                    buf.at[t],
                    buf.at[t],
                    ag_send.at[a, k],
                    ag_recv.at[a, t],
                    "tp",
                    tp_at(k) * 2 + c,
                )
            )
        launch(remote(buf.at[t], buf.at[t], ag_send.at[a, 0], ag_recv.at[a, t], "tp", peer))

    def gather_wait(a, buf, slot):
        remote(
            buf.at[slot], buf.at[slot], ag_send.at[a, 0], ag_recv.at[a, slot], "tp", peer
        ).wait_recv()

    def gather_forward(a, buf):
        for k in range(1, X):
            slot = tp_from(k) * 2 + c
            gather_wait(a, buf, slot)
            launch(
                remote(
                    buf.at[slot],
                    buf.at[slot],
                    ag_send.at[a, X - 1 + k],
                    ag_recv.at[a, slot],
                    "tp",
                    peer,
                )
            )

    def gather_finish(a, buf):
        gather_forward(a, buf)
        for k in range(X):
            gather_wait(a, buf, tp_from(k) * 2 + other)

    def project_source(layer, at):
        rows = xs[pl.ds(2 * at, 2)].reshape(2 * Rs, D)

        def one(j, carry):
            kv[j, at] = mm(rows, wkv[j]).astype(BF)
            return carry

        lax.fori_loop(2 * layer, 2 * layer + 2, one, 0)

    def query_copy(layer, i, block, where):
        return remote(
            qall.at[layer, block],
            qall.at[layer, block],
            q_send.at[layer, i],
            q_recv.at[layer, block],
            "sp",
            where,
        )

    def send_queries(layer):
        load_q[layer].wait()
        rows = xt[layer].reshape(T, D)
        qall[layer, s] = mm(rows, wq[layer]).astype(BF)
        for i in range(1, S):
            launch(query_copy(layer, i, s, sp_at(i)))

    def attend_block(layer, block, sums, stats):
        lanes = lax.broadcasted_iota(jnp.int32, (T, LANES), 1)
        packed = jnp.zeros((T, LANES), F32)
        for h in range(heads):
            cols = slice(h * HD, (h + 1) * HD)
            query = qall[layer, block, :, cols]
            keys = kv[2 * layer, :, :, cols].reshape(n * Rs, HD)
            values = kv[2 * layer + 1, :, :, cols].reshape(n * Rs, HD)
            scores = (
                lax.dot_general(query, keys, (((1,), (1,)), ((), ())), preferred_element_type=F32)
                * scale
            )
            top = jnp.max(scores, axis=-1, keepdims=True)
            raised = jnp.exp(scores - top)
            total = jnp.sum(raised, axis=-1, keepdims=True)
            sums[:, cols] = mm(raised.astype(BF), values).astype(BF)
            packed = jnp.where(lanes == 2 * h, top, packed)
            packed = jnp.where(lanes == 2 * h + 1, total, packed)
        stats[...] = packed.T[:STAT_ROWS]

    def sums_copy(layer, i, slot, block):
        return remote(
            osend.at[layer, i],
            orecv.at[layer, slot],
            r_send.at[layer, i],
            r_recv.at[layer, slot],
            "sp",
            block,
        )

    def stats_copy(layer, i, slot, block):
        return remote(
            ssend.at[layer, i],
            srecv.at[layer, slot],
            s_send.at[layer, i],
            s_recv.at[layer, slot],
            "sp",
            block,
        )

    def attend(layer, meanwhile):
        attend_block(layer, s, orecv.at[layer, s], srecv.at[layer, s])

        def one(i, carry):
            block = sp_at(i)
            query_copy(layer, 0, block, block).wait_recv()
            attend_block(layer, block, osend.at[layer, block], ssend.at[layer, block])
            sums_copy(layer, block, s, block).start()
            stats_copy(layer, block, s, block).start()
            return carry

        lax.fori_loop(1, S, one, 0)
        meanwhile()

        def wait_block(i, carry):
            block = sp_at(i)
            sums_copy(layer, block, block, block).wait_recv()
            stats_copy(layer, block, block, block).wait_recv()
            return carry

        lax.fori_loop(1, S, wait_block, 0)
        rows = srecv[layer].reshape(S * STAT_ROWS, T)
        if S * STAT_ROWS < LANES:
            rows = jnp.concatenate([rows, jnp.zeros((LANES - S * STAT_ROWS, T), F32)], axis=0)
        stats = rows.T
        for h in range(heads):
            cols = slice(h * HD, (h + 1) * HD)
            tops = [stats[:, b * STAT_ROWS + 2 * h :][:, :1] for b in range(S)]
            highest = functools.reduce(jnp.maximum, tops)
            total = jnp.zeros((T, 1), F32)
            summed = jnp.zeros((T, HD), F32)
            for b in range(S):
                factor = jnp.exp(tops[b] - highest)
                total = total + factor * stats[:, b * STAT_ROWS + 2 * h + 1 :][:, :1]
                summed = summed + factor * orecv[layer, b, :, cols].astype(F32)
            att[:, cols] = (summed / total).astype(BF)
        load_o[layer].wait()
        spread_sum(layer, att, wo.at[layer])

    def spread_sum(a, lhs, weight):
        def one(j, carry):
            cols = pl.ds(pl.multiple_of(j * TILE, TILE), TILE)
            pf[:, :, cols] = mm(lhs[...], weight[:, cols]).reshape(n, Rt, TILE)
            return carry

        lax.fori_loop(0, D // TILE, one, 0)
        order = [*range(1, X), 0]

        def first(k):
            return remote(
                p1s.at[a, k], p1r.at[a, k], p1_send.at[a, k], p1_recv.at[a, k], "tp", peer
            )

        def second(k):
            return remote(
                p2s.at[a, k],
                p2r.at[a, k],
                p2_send.at[a, k],
                p2_recv.at[a, k],
                "tp",
                tp_at(k) * 2 + c,
            )

        for k in order:
            p1s[a, k] = pf[tp_at(k) * 2 + other].astype(BF)
            launch(first(k))
        for k in range(1, X):
            first(k).wait_recv()
            p2s[a, k] = (pf[tp_at(k) * 2 + c] + p1r[a, k].astype(F32)).astype(BF)
            launch(second(k))
        first(0).wait_recv()
        own = pf[t] + p1r[a, 0].astype(F32)
        for k in range(1, X):
            second(k).wait_recv()
            own = own + p2r[a, k].astype(F32)
        residual[...] = residual[...] + own

    load_t.wait()
    residual[...] = tv[...].astype(F32)
    xt[0, t] = normed_rows(residual[...], attend_gain[0:1]).astype(BF)
    pl.semaphore_wait(barrier, X + S - 1)
    gather_start(0, xt.at[0])
    for copy in load_kv[0]:
        copy.start()
    load_s.wait()
    step = 32

    def norm_source(j, carry):
        rows = pl.ds(pl.multiple_of(j * step, step), step)
        xs[t, rows] = normed_rows(sv[rows].astype(F32), source_gain[...]).astype(BF)
        return carry

    lax.fori_loop(0, Rs // step, norm_source, 0)
    gather_start(3, xs)
    gather_finish(0, xt.at[0])
    send_queries(0)
    for copy in [*load_kv[1], load_o[0], load_q[1], load_o[1]]:
        copy.start()
    for copy in load_kv[0]:
        copy.wait()
    gather_wait(3, xs, peer)
    project_source(0, x)
    for copy in load_kv[1]:
        copy.wait()
    project_source(1, x)
    for copy in load_m:
        copy.start()
    gather_forward(3, xs)
    for k in range(1, X):
        gather_wait(3, xs, tp_from(k) * 2 + other)
        project_source(0, tp_from(k))

    def rest_of_source():
        for k in range(1, X):
            project_source(1, tp_from(k))

    attend(0, rest_of_source)
    xt[1, t] = normed_rows(residual[...], attend_gain[1:2]).astype(BF)
    gather_start(1, xt.at[1])
    gather_finish(1, xt.at[1])
    send_queries(1)
    attend(1, lambda: None)
    xt[2, t] = normed_rows(residual[...], mixer_gain[...]).astype(BF)
    gather_start(2, xt.at[2])
    gather_finish(2, xt.at[2])
    load_m[0].wait()
    load_m[1].wait()
    mixed = xt[2].reshape(T, D)
    pads = ((gpad, wg), (upad, wu))

    def halo_out(number):
        return remote(
            hs.at[number],
            hr.at[number],
            h_send.at[number],
            h_recv.at[number],
            "sp",
            lax.rem(s + 1, S),
        )

    for number, (pad, weight) in enumerate(pads):
        lifted = (
            lax.dot_general(
                mixed, weight[...], (((1,), (1,)), ((), ())), preferred_element_type=F32
            )
            .astype(BF)
            .astype(F32)
        )
        hs[number] = lifted[T - 8 :]

        @pl.when(s < S - 1)
        def _():
            halo_out(number).start()

        pad[8:] = lifted

    def hidden_rows(start, stop):
        def convolved(pad, taps):
            return (
                taps[0:1] * pad[6 + start : 6 + stop]
                + taps[1:2] * pad[7 + start : 7 + stop]
                + taps[2:3] * pad[8 + start : 8 + stop]
            )

        gate = convolved(gpad, gate_taps)
        hid[start:stop] = (gate / (1.0 + jnp.exp(-gate)) * convolved(upad, up_taps)).astype(BF)

    hidden_rows(16, T)

    @pl.when(s == 0)
    def _():
        for pad, _weight in pads:
            pad[:8] = jnp.zeros((8, F), F32)

    @pl.when(s > 0)
    def _():
        for number, (pad, _weight) in enumerate(pads):
            halo_out(number).wait_recv()
            pad[:8] = hr[number]

    @pl.when(s < S - 1)
    def _():
        for number in range(2):
            halo_out(number).wait_send()

    hidden_rows(0, 16)
    load_m[2].wait()
    spread_sum(2, hid, wd)
    result[...] = normed_rows(residual[...], final_gain[...]).astype(BF)
    for copy in pending:
        copy.wait_send()
    for layer in range(2):

        def wait_sent(i, carry):
            block = sp_at(i)
            sums_copy(layer, block, s, block).wait_send()
            stats_copy(layer, block, s, block).wait_send()
            return carry

        lax.fori_loop(1, S, wait_sent, 0)


def body(n, S, *arrays):
    (
        source,
        target,
        source_gain,
        attend_gain,
        query_weight,
        key_weight,
        value_weight,
        out_weight,
        mixer_gain,
        gate_weight,
        up_weight,
        gate_taps,
        up_taps,
        down_weight,
        final_gain,
    ) = arrays
    Rs, D = source.shape
    Rt = target.shape[0]
    W = query_weight.shape[2]
    F = gate_weight.shape[1]
    T = n * Rt
    X = n // 2
    hbm = pl.BlockSpec(memory_space=pl.ANY)
    vmem = pl.BlockSpec(memory_space=pltpu.VMEM)
    dma = pltpu.SemaphoreType.DMA
    scratch = [
        pltpu.VMEM((Rs, D), BF),
        pltpu.VMEM((Rt, D), BF),
        pltpu.VMEM((2, D, W), BF),
        pltpu.VMEM((4, D, W), BF),
        pltpu.VMEM((2, W, D), BF),
        pltpu.VMEM((F, D), BF),
        pltpu.VMEM((F, D), BF),
        pltpu.VMEM((F, D), BF),
        pltpu.VMEM((n, Rs, D), BF),
        pltpu.VMEM((3, n, Rt, D), BF),
        pltpu.VMEM((4, X, 2 * Rs, W), BF),
        pltpu.VMEM((2, S, T, W), BF),
        pltpu.VMEM((2, S, T, W), BF),
        pltpu.VMEM((2, S, T, W), BF),
        pltpu.VMEM((2, S, STAT_ROWS, T), F32),
        pltpu.VMEM((2, S, STAT_ROWS, T), F32),
        pltpu.VMEM((n, Rt, D), F32),
        pltpu.VMEM((T, W), BF),
        pltpu.VMEM((3, X, Rt, D), BF),
        pltpu.VMEM((3, X, Rt, D), BF),
        pltpu.VMEM((3, X, Rt, D), BF),
        pltpu.VMEM((3, X, Rt, D), BF),
        pltpu.VMEM((2, 8, F), F32),
        pltpu.VMEM((2, 8, F), F32),
        pltpu.VMEM((T + 8, F), F32),
        pltpu.VMEM((T + 8, F), F32),
        pltpu.VMEM((T, F), BF),
        pltpu.VMEM((Rt, D), F32),
        dma((2,)),
        dma((11,)),
        dma((4, n)),
        dma((4, n)),
        dma((2, S)),
        dma((2, S)),
        dma((2, S)),
        dma((2, S)),
        dma((2, S)),
        dma((2, S)),
        dma((3, X)),
        dma((3, X)),
        dma((3, X)),
        dma((3, X)),
        dma((2,)),
        dma((2,)),
    ]
    return pl.pallas_call(
        functools.partial(kernel, n, S),
        out_shape=jax.ShapeDtypeStruct((Rt, D), BF),
        in_specs=[
            hbm,
            hbm,
            vmem,
            vmem,
            hbm,
            hbm,
            hbm,
            hbm,
            vmem,
            hbm,
            hbm,
            vmem,
            vmem,
            hbm,
            vmem,
        ],
        out_specs=vmem,
        scratch_shapes=scratch,
        compiler_params=pltpu.CompilerParams(
            collective_id=0, has_side_effects=True, vmem_limit_bytes=67043328
        ),
    )(
        source,
        target,
        source_gain.reshape(1, D),
        attend_gain,
        query_weight,
        key_weight,
        value_weight,
        out_weight,
        mixer_gain.reshape(1, D),
        gate_weight.T,
        up_weight.T,
        gate_taps,
        up_taps,
        down_weight,
        final_gain.reshape(1, D),
    )


def solution(mesh):
    placed = (
        P(("grp", "sp", "tp"), None),
        P(("grp", "sp", "tp"), None),
        P(),
        P(),
        P(None, None, "tp"),
        P(None, None, "tp"),
        P(None, None, "tp"),
        P(None, "tp", None),
        P(),
        P(None, "tp"),
        P(None, "tp"),
        P(None, "tp"),
        P(None, "tp"),
        P("tp", None),
        P(),
    )
    return jax.shard_map(
        functools.partial(body, mesh.shape["tp"], mesh.shape["sp"]),
        mesh=mesh,
        in_specs=placed,
        out_specs=P(("grp", "sp", "tp"), None),
        check_vma=False,
    )
```
